256 devices in a mesh: grp: 2 (over y), sp: 32 (over z, core), tp: 4 (over x).
Axes of the slice: x: 4, y: 2, z: 16, core: 2. Of those that a mesh axis runs over, the one named last changes fastest.
The devices are a block of a 4x16x16 slice.
Arguments:
- residual: bfloat16 [49152, 2048], P(('grp', 'sp', 'tp')), parts along dimension 0, may hold values from -6 to 6
- value_projected: bfloat16 [49152, 4096], P(('grp', 'sp'), 'tp'), parts along dimension 0, may hold values from -6 to 6
- gate_projected: bfloat16 [49152, 4096], P(('grp', 'sp'), 'tp'), parts along dimension 0, may hold values from -6 to 6
- wide_key_rows: bfloat16 [49152, 1024], P(('grp', 'sp'), 'tp'), parts along dimension 0, may hold values from -6 to 6
- wide_query_rows: bfloat16 [49152, 1024], P(('grp', 'sp'), 'tp'), parts along dimension 0, may hold values from -6 to 6
- narrow_key_rows: bfloat16 [49152, 512], P(('grp', 'sp'), 'tp'), parts along dimension 0, may hold values from -6 to 6
- narrow_query_rows: bfloat16 [49152, 512], P(('grp', 'sp'), 'tp'), parts along dimension 0, may hold values from -6 to 6
- step_before_softplus: float32 [49152, 64], P(('grp', 'sp'), 'tp'), parts along dimension 0, may hold values from -5 to 5
- extra_log_decay: float32 [49152, 64], P(('grp', 'sp'), 'tp'), parts along dimension 0, may hold values from -0.7 to 0
- log_decay_rate: float32 [64], P('tp'), may hold values from -12.3 to -2.99
- value_kernel: bfloat16 [4, 4096], P(None, 'tp'), may hold values from -3 to 3
- wide_key_kernel: bfloat16 [4, 1024], P(None, 'tp'), may hold values from -3 to 3
- wide_query_kernel: bfloat16 [4, 1024], P(None, 'tp'), may hold values from -3 to 3
- narrow_key_kernel: bfloat16 [4, 512], P(None, 'tp'), may hold values from -3 to 3
- narrow_query_kernel: bfloat16 [4, 512], P(None, 'tp'), may hold values from -3 to 3
- head_norm_gain: bfloat16 [4096], P('tp'), may hold values from 0.099609375 to 1.8984375
- output_matrix: bfloat16 [4096, 2048], P('tp'), may hold values from -0.09375 to 0.09375
- feedforward_norm_gain: bfloat16 [2048], replicated, may hold values from 0.099609375 to 1.8984375
- gate_matrix: bfloat16 [2048, 3072], P('sp', 'tp'), may hold values from -0.125 to 0.125
- up_matrix: bfloat16 [2048, 3072], P('sp', 'tp'), may hold values from -0.125 to 0.125
- down_matrix: bfloat16 [2048, 3072], P('sp', 'tp'), may hold values from -0.3125 to 0.3125
Outputs:
- mixed: bfloat16 [49152, 2048], P(('grp', 'sp', 'tp')), parts along dimension 0
The draws below stay inside these ranges and needn't reach their ends.
There are 2 independent parts, one for each index of `grp`. The reference program is written for one: setup_inputs(seed, part) draws one part's arguments, and reference() takes and returns one part's arrays. A program takes and returns all parts, laid end to end along the dimension named above; an argument that names none is the same for every part. Nothing has to cross between parts.
All inputs are finite; a program needn't handle non-finite values.
Results may differ from the reference program's by a relative error of at most 0.015.
Values may be sent and summed in bfloat16 or wider, within the bound.
No kernel may reach another device: no remote copies, remote signals or barrier semaphores. Data moves between devices by JAX's collectives and lax.ppermute only.
A program may use at most 128 MiB of HBM per device.

```python
import math
import jax
import jax.numpy as jnp
from jax import lax

D = 2048
HEADS = 64
HEAD_DIM = 64
GROUPS = 16
STATE_WIDE = 128
STATE_NARROW = 64
FF = 3072
CONV_W = 4
BLK = 64
TOK_DEV = 768
INNER = 4096
TOKENS = 24576
N_TP = 4


def draw_step_before_softplus(key, part):
    noise_key, shift_key = jax.random.split(jax.random.fold_in(key, 11))
    count = TOKENS // TOK_DEV
    shifts = jax.random.uniform(shift_key, (count, 1, HEADS), jnp.float32, -1.0, 1.0)
    noise = jnp.clip(jax.random.normal(noise_key, (count, TOK_DEV, HEADS), jnp.float32), -4.0, 4.0)
    return (noise + shifts).reshape(TOKENS, HEADS)


def draw_extra_log_decay(key, part):
    place_key, loss_key = jax.random.split(jax.random.fold_in(key, 23))
    places = jax.random.randint(place_key, (2, HEADS), 0, TOKENS)
    losses = jax.random.uniform(loss_key, (2, HEADS), jnp.float32, 0.2, 0.5)
    positions = jnp.arange(TOKENS, dtype=jnp.int32)[:, None]
    total = jnp.zeros((TOKENS, HEADS), jnp.float32)
    for number in range(2):
        total = total + jnp.where(positions == places[number][None, :], jnp.log(1.0 - losses[number])[None, :], 0.0)
    return total


def draw_log_decay_rate(key, part):
    order_key, slow_key, fast_key = jax.random.split(jax.random.fold_in(key, 37), 3)
    order = jax.random.permutation(order_key, HEADS)
    fast_count = HEADS // 2
    slow = math.log(5e-06) + jax.random.uniform(slow_key, (HEADS,), jnp.float32) * math.log(4.0)
    fast = math.log(0.03) + jax.random.uniform(fast_key, (HEADS,), jnp.float32) * math.log(0.05 / 0.03)
    return jnp.where(order < fast_count, fast, slow)


def steps_of(key, extent, shards, least, top_value):
    level = 1.0
    for position, blocks in shards:
        draws = jax.random.uniform(jax.random.fold_in(jax.random.fold_in(key, 6), position), (blocks,), jnp.float32, least / len(shards), top_value / len(shards))
        level = level * jnp.repeat(jnp.exp(draws), extent[position] // blocks).reshape((-1,) + (1,) * (len(extent) - 1 - position))
    return level


def normal_values(own_key, dims, scale, bound, shards=(), kind=jnp.bfloat16):
    result = jax.random.normal(own_key, dims, jnp.float32) * scale
    if len(shards) > 0:
        result = steps_of(own_key, dims, shards, -0.22, 0.18) * result
    return jnp.clip(result, min=-bound, max=bound).astype(kind)


def setup_inputs(seed: int = 0, part: int = 0) -> dict:
    seeds = jax.random.split(jax.random.key(seed), 22)
    part_keys = jax.random.split(jax.random.fold_in(seeds[21], part), 22)
    return {
        "residual": normal_values(part_keys[0], (TOKENS, D), 1.0, 6.0, ((0, 128),)),
        "value_projected": normal_values(part_keys[1], (TOKENS, INNER), 1.0, 6.0, ((0, 32), (1, 4))),
        "gate_projected": normal_values(part_keys[2], (TOKENS, INNER), 1.0, 6.0, ((0, 32), (1, 4))),
        "wide_key_rows": normal_values(part_keys[3], (TOKENS, GROUPS * STATE_WIDE // 2), 1.0, 6.0, ((0, 32), (1, 4))),
        "wide_query_rows": normal_values(part_keys[4], (TOKENS, GROUPS * STATE_WIDE // 2), 1.0, 6.0, ((0, 32), (1, 4))),
        "narrow_key_rows": normal_values(part_keys[5], (TOKENS, GROUPS * STATE_NARROW // 2), 1.0, 6.0, ((0, 32), (1, 4))),
        "narrow_query_rows": normal_values(part_keys[6], (TOKENS, GROUPS * STATE_NARROW // 2), 1.0, 6.0, ((0, 32), (1, 4))),
        "step_before_softplus": draw_step_before_softplus(jax.random.fold_in(jax.random.fold_in(seeds[21], part), 71), part),
        "extra_log_decay": draw_extra_log_decay(jax.random.fold_in(jax.random.fold_in(seeds[21], part), 71), part),
        "log_decay_rate": draw_log_decay_rate(jax.random.fold_in(seeds[21], 71), part),
        "value_kernel": normal_values(seeds[10], (CONV_W, INNER), CONV_W ** -0.5, 3.0, ((1, 4),)),
        "wide_key_kernel": normal_values(seeds[11], (CONV_W, GROUPS * STATE_WIDE // 2), CONV_W ** -0.5, 3.0, ((1, 4),)),
        "wide_query_kernel": normal_values(seeds[12], (CONV_W, GROUPS * STATE_WIDE // 2), CONV_W ** -0.5, 3.0, ((1, 4),)),
        "narrow_key_kernel": normal_values(seeds[13], (CONV_W, GROUPS * STATE_NARROW // 2), CONV_W ** -0.5, 3.0, ((1, 4),)),
        "narrow_query_kernel": normal_values(seeds[14], (CONV_W, GROUPS * STATE_NARROW // 2), CONV_W ** -0.5, 3.0, ((1, 4),)),
        "head_norm_gain": jnp.clip(1.0 + 0.18 * jax.random.normal(seeds[15], (INNER,), jnp.float32), 0.099609375, 1.8984375).astype(jnp.bfloat16),
        "output_matrix": normal_values(seeds[16], (INNER, D), INNER ** -0.5, 0.09375, ((0, 4),)),
        "feedforward_norm_gain": jnp.clip(1.0 + 0.18 * jax.random.normal(seeds[17], (D,), jnp.float32), 0.099609375, 1.8984375).astype(jnp.bfloat16),
        "gate_matrix": normal_values(seeds[18], (D, FF), D ** -0.5, 0.125, ((0, 32), (1, 4))),
        "up_matrix": normal_values(seeds[19], (D, FF), D ** -0.5, 0.125, ((0, 32), (1, 4))),
        "down_matrix": normal_values(seeds[20], (D, FF), (FF // 9) ** -0.5, 0.3125, ((0, 32), (1, 4))),
    }


def to_half(value):
    return lax.optimization_barrier(value.astype(jnp.bfloat16)).astype(jnp.float32)

def short_conv(inputs, kernel):
    width = kernel.shape[0]
    length = inputs.shape[0]
    padded = jnp.pad(inputs.astype(jnp.float32), ((width - 1, 0), (0, 0)))
    total = jnp.zeros(inputs.shape, jnp.float32)
    for offset in range(width):
        total = total + padded[offset:offset + length] * kernel[offset].astype(jnp.float32)
    return jax.nn.silu(total).astype(jnp.bfloat16)

def family_mix(values, step_sizes, decay_factor, keys, queries):
    length, groups, per_group, width = values.shape
    states = keys.shape[2]
    count = length // BLK
    lower = jnp.tril(jnp.ones((BLK, BLK), dtype=bool))
    highest = lax.Precision.HIGHEST

    def advance(carried, block):
        block_values, block_steps, block_decay, block_keys, block_queries = block
        values32 = block_values.astype(jnp.float32)
        keys32 = block_keys.astype(jnp.float32)
        queries32 = block_queries.astype(jnp.float32)
        running = jnp.cumsum(block_decay, axis=0)
        scores = jnp.einsum('lgn,sgn->lsg', queries32, keys32, precision=highest)
        spread = jnp.where(lower[:, :, None, None], running[:, None] - running[None, :], -jnp.inf)
        weights = to_half(scores[..., None] * jnp.exp(spread) * block_steps[None])
        inside = jnp.einsum('lsgr,sgrp->lgrp', weights, values32, precision=highest)
        outside = jnp.exp(running)[..., None] * jnp.einsum('lgn,grpn->lgrp', queries32, to_half(carried), precision=highest)
        fade = block_steps * jnp.exp(running[-1][None] - running)
        scaled = to_half(values32 * fade[..., None])
        block_state = jnp.einsum('lgrp,lgn->grpn', scaled, keys32, precision=highest)
        carried = jnp.exp(running[-1])[..., None, None] * carried + block_state
        return (carried, inside + outside)
    blocks = (values.reshape(count, BLK, groups, per_group, width), step_sizes.reshape(count, BLK, groups, per_group), decay_factor.reshape(count, BLK, groups, per_group), keys.reshape(count, BLK, groups, states), queries.reshape(count, BLK, groups, states))
    initial = jnp.zeros((groups, per_group, width, states), jnp.float32)
    ending, outputs = lax.scan(advance, initial, blocks)
    return outputs.reshape(length, groups, per_group, width)

def reference(residual, value_projected, gate_projected, wide_key_rows, wide_query_rows, narrow_key_rows, narrow_query_rows, step_before_softplus, extra_log_decay, log_decay_rate, value_kernel, wide_key_kernel, wide_query_kernel, narrow_key_kernel, narrow_query_kernel, head_norm_gain, output_matrix, feedforward_norm_gain, gate_matrix, up_matrix, down_matrix):
    length = value_projected.shape[0]
    per_group = HEADS // GROUPS
    half = GROUPS // 2
    values = short_conv(value_projected, value_kernel).reshape(length, half, 2, per_group, HEAD_DIM)
    keys_w = short_conv(wide_key_rows, wide_key_kernel).reshape(length, half, STATE_WIDE)
    queries_w = short_conv(wide_query_rows, wide_query_kernel).reshape(length, half, STATE_WIDE)
    keys_n = short_conv(narrow_key_rows, narrow_key_kernel).reshape(length, half, STATE_NARROW)
    queries_n = short_conv(narrow_query_rows, narrow_query_kernel).reshape(length, half, STATE_NARROW)
    step_sizes = jax.nn.softplus(step_before_softplus)
    decay_factor = -jnp.exp(log_decay_rate)[None, :] * step_sizes + extra_log_decay
    step_sizes = step_sizes.reshape(length, half, 2, per_group)
    decay_factor = decay_factor.reshape(length, half, 2, per_group)
    wide = family_mix(values[:, :, 0], step_sizes[:, :, 0], decay_factor[:, :, 0], keys_w, queries_w)
    narrow = family_mix(values[:, :, 1], step_sizes[:, :, 1], decay_factor[:, :, 1], keys_n, queries_n)
    heads_out = jnp.stack([wide, narrow], axis=2).reshape(length, HEADS, HEAD_DIM)
    gated = heads_out * jax.nn.silu(gate_projected.astype(jnp.float32)).reshape(length, HEADS, HEAD_DIM)
    gated = gated * lax.rsqrt(lax.optimization_barrier(jnp.mean(gated * gated, axis=-1, keepdims=True)) + 1e-06)
    normed = (gated.reshape(length, INNER) * head_norm_gain.astype(jnp.float32)).astype(jnp.bfloat16)
    share = INNER // N_TP
    projected = jnp.zeros((length, D), jnp.float32)
    for index in range(N_TP):
        partial_value = jnp.dot(normed[:, index * share:(index + 1) * share], output_matrix[index * share:(index + 1) * share], preferred_element_type=jnp.float32)
        projected = projected + to_half(partial_value)
    after_mixer = (residual.astype(jnp.float32) + projected).astype(jnp.bfloat16)
    rows = after_mixer.astype(jnp.float32)
    x_norm = (rows * lax.rsqrt(lax.optimization_barrier(jnp.mean(rows * rows, axis=-1, keepdims=True)) + 1e-06) * feedforward_norm_gain.astype(jnp.float32)).astype(jnp.bfloat16)
    gate_values = jnp.dot(x_norm, gate_matrix, preferred_element_type=jnp.float32)
    up_values = jnp.dot(x_norm, up_matrix, preferred_element_type=jnp.float32)
    hidden = (jax.nn.silu(gate_values) * up_values).astype(jnp.bfloat16)
    portion = FF // N_TP
    channel = jnp.zeros((length, D), jnp.float32)
    for index in range(N_TP):
        partial_value = lax.dot_general(hidden[:, index * portion:(index + 1) * portion], down_matrix[:, index * portion:(index + 1) * portion], (((1,), (1,)), ((), ())), preferred_element_type=jnp.float32)
        channel = channel + to_half(partial_value)
    return (after_mixer.astype(jnp.float32) + 0.5 * channel).astype(jnp.bfloat16)
```

```python
import functools

import jax
import jax.numpy as jnp
import numpy as np
from jax import lax
from jax.experimental import pallas as pl
from jax.experimental.pallas import tpu as pltpu
from jax.sharding import PartitionSpec as P


CH = 64
PER = 4
GW = PER * CH
BT = 128
WIDE = 128
NARROW = 64
TAPS = 4
EDGE = 8
EPS = 1e-6
F32 = jnp.float32
BF16 = jnp.bfloat16
VMEM_LIMIT = 60 << 20
SMALL_LIMIT = 12 << 20
FEED_LIMIT = 24 << 20


def dot(a, b):
    return jnp.dot(a, b, preferred_element_type=F32)


def dot_nt(a, b):
    return lax.dot_general(a, b, (((1,), (1,)), ((), ())), preferred_element_type=F32)


def dot_tn(a, b):
    return lax.dot_general(a, b, (((0,), (0,)), ((), ())), preferred_element_type=F32)


def halves(x):
    hi = x.astype(BF16)
    return hi, (x - hi.astype(F32)).astype(BF16)


def dot2(pair, b):
    return dot(pair[0], b) + dot(pair[1], b)


def silu(x):
    h = 0.5 * x
    return h + h * jnp.tanh(h)


def group_rows(groups):
    out, row = [], 0
    wide_cols = (groups // 2) * WIDE
    for g in range(groups):
        size = NARROW if g % 2 else WIDE
        key = wide_cols + (g // 2) * NARROW if g % 2 else (g // 2) * WIDE
        out.append((row, size, key))
        row += size
    return out, row


def conv_cols(buf, cols, ker):
    k = ker.astype(F32)
    first = EDGE - TAPS + 1
    total = buf[first : first + BT, cols] * k[0:1]
    for tap in range(1, TAPS):
        total += buf[first + tap : first + tap + BT, cols] * k[tap : tap + 1]
    return silu(total)


def edge_kernel(*refs):
    ins, (edge, both) = refs[:-2], refs[-2:]
    at = 0
    for part in ins[:-3]:
        edge[:, at : at + part.shape[1]] = part[...]
        at += part.shape[1]
    at = 0
    for part in ins[-3:]:
        both[:, at : at + part.shape[1]] = part[...]
        at += part.shape[1]


def states_kernel(
    groups, chunk, rim, value, wk, nk, step, extra, rate, kv, kwk, knk, table, place, pick,
    up, kk, er, eR, hs, st, bufv, bufk, state, before,
):
    i = pl.program_id(0)
    info, _ = group_rows(groups)
    inner, wcols, ncols = value.shape[1], wk.shape[1], nk.shape[1]

    @pl.when(i == 0)
    def _():
        bufv[0:EDGE, :] = rim[:, 0:inner].astype(F32)
        bufk[0:EDGE, :] = rim[:, inner : inner + wcols + ncols].astype(F32)
        state[...] = jnp.zeros_like(state)
        before[...] = jnp.zeros_like(before)

    bufv[EDGE:, :] = value[...].astype(F32)
    bufk[EDGE:, 0:wcols] = wk[...].astype(F32)
    bufk[EDGE:, wcols:] = nk[...].astype(F32)

    heads = step.shape[0]
    diagonal = lax.broadcasted_iota(jnp.int32, (heads, heads), 0) == lax.broadcasted_iota(
        jnp.int32, (heads, heads), 1
    )
    speed = jnp.exp(jnp.sum(jnp.where(diagonal, rate[...], 0.0), axis=1, keepdims=True))
    dt = jnp.log(1.0 + jnp.exp(step[...]))
    a = extra[...] - speed * dt
    upto = lax.broadcasted_iota(jnp.int32, (BT, BT), 0) <= lax.broadcasted_iota(
        jnp.int32, (BT, BT), 1
    )
    upto = jnp.where(upto, 1.0, 0.0).astype(BF16)
    a1 = a.astype(BF16)
    a2, a3 = halves(a - a1.astype(F32))
    r = dot(a1, upto) + dot(a2, upto) + dot(a3, upto)
    mid, end = r[:, BT // 2 - 1 : BT // 2], r[:, BT - 1 : BT]
    er[...] = jnp.exp(r - mid).T
    eR[...] = jnp.exp(r + before[...]).T
    before[...] = before[...] + end
    inward = halves((jnp.exp(mid - r) * dt).T)
    lane = lax.broadcasted_iota(jnp.int32, r.shape, 1)
    scales = jnp.exp(jnp.where(lane == 0, mid, jnp.where(lane == 1, end, end - mid)))
    scales = halves(scales.T[0:8])

    for c in range(0, wcols, 128):
        cols = slice(c, c + 128)
        kk[:, cols] = conv_cols(bufk, cols, kwk[:, cols]).astype(BF16)
    for c in range(0, ncols, 128):
        cols = slice(wcols + c, wcols + c + 128)
        kk[:, cols] = conv_cols(bufk, cols, knk[:, c : c + 128]).astype(BF16)
    for g, (row, size, key) in enumerate(info):
        cols = slice(g * GW, (g + 1) * GW)
        tab = table[:, cols]
        f = dot2(inward, tab)
        s = dot2(scales, tab)
        u = conv_cols(bufv, cols, kv[:, cols]).astype(BF16).astype(F32)
        scaled = (u * f).astype(BF16)
        up[:, cols] = scaled
        added = dot_tn(kk[:, key : key + size], scaled)
        old = state[row : row + size, :]
        hs[0, row : row + size, :] = (old * s[0:1]).astype(BF16)
        state[row : row + size, :] = old * s[1:2] + added * s[2:3]
    bufv[0:EDGE, :] = bufv[BT:, :]
    bufk[0:EDGE, :] = bufk[BT:, :]

    @pl.when(i == pl.num_programs(0) - 1)
    def _():
        total = halves(before[...].T[0:8])
        line_t = (dot(total[0], place[:, 0:GW]) + dot(total[1], place[:, GW:]))[0:1]
        sent = dot(pick[...], state[...].astype(BF16))
        used, padded = chunk
        rows = lax.broadcasted_iota(jnp.int32, sent.shape, 0)
        st[...] = jnp.where(rows % padded == used, line_t, sent).astype(BF16)


def inner_kernel(groups, rim, wq, nq, kwq, knq, kk, up, er, hs, table, yl, qq, bufq):
    i = pl.program_id(0)
    info, _ = group_rows(groups)
    wcols, ncols = wq.shape[1], nq.shape[1]

    @pl.when(i == 0)
    def _():
        bufq[0:EDGE, :] = rim[:, rim.shape[1] - wcols - ncols :].astype(F32)

    bufq[EDGE:, 0:wcols] = wq[...].astype(F32)
    bufq[EDGE:, wcols:] = nq[...].astype(F32)
    for c in range(0, wcols, 128):
        cols = slice(c, c + 128)
        qq[:, cols] = conv_cols(bufq, cols, kwq[:, cols]).astype(BF16)
    for c in range(0, ncols, 128):
        cols = slice(wcols + c, wcols + c + 128)
        qq[:, cols] = conv_cols(bufq, cols, knq[:, c : c + 128]).astype(BF16)
    bufq[0:EDGE, :] = bufq[BT:, :]
    outward = halves(er[...])
    t = lax.broadcasted_iota(jnp.int32, (BT, BT), 0)
    s = lax.broadcasted_iota(jnp.int32, (BT, BT), 1)
    for g, (row, size, key) in enumerate(info):
        cols = slice(g * GW, (g + 1) * GW)
        q, k = qq[:, key : key + size], kk[:, key : key + size]
        weights = jnp.where(s <= t, dot_nt(q, k), 0.0).astype(BF16)
        y = dot(weights, up[:, cols]) + dot(q, hs[0, row : row + size, :])
        yl[:, cols] = y * dot2(outward, table[:, cols])


def row_fades(groups, used, padded, place, sums, table):
    info, _ = group_rows(groups)
    factor = halves(jnp.exp(sums))
    fades = [dot2(factor, table[:, g * GW : (g + 1) * GW]) for g in range(groups)]
    row = lax.broadcasted_iota(jnp.int32, (padded, GW), 0) + place * used
    masks = [row >= info[g][0] for g in range(1, groups)]

    def fade(k):
        out = jnp.broadcast_to(fades[0][k : k + 1], (padded, GW))
        for g in range(1, groups):
            out = jnp.where(masks[g - 1], fades[g][k : k + 1], out)
        return out

    return fade


def near_kernel(groups, chunk, where_ref, got, gather, unplace, place, table, prefix, sums, sent):
    used, padded = chunk
    count = got.shape[0] // padded
    lines = dot(gather[...], got[...]).astype(BF16)
    logs = dot(lines, unplace[...])
    sums[...] = logs
    fade = row_fades(groups, used, padded, where_ref[0], logs, table)
    held = jnp.zeros((padded, GW), F32)
    for k in range(count):
        part = slice(k * padded, (k + 1) * padded)
        prefix[part, :] = held
        held = fade(k) * held + got[part, :].astype(F32)
    total = halves(jnp.broadcast_to(jnp.sum(logs, axis=0, keepdims=True), (8, logs.shape[1])))
    line = (dot(total[0], place[:, 0:GW]) + dot(total[1], place[:, GW:]))[0:1]
    row = lax.broadcasted_iota(jnp.int32, held.shape, 0)
    sent[...] = jnp.where(row == used, line, held).astype(BF16)


def far_kernel(groups, chunk, where_ref, prefix, sums, unplace, table, *refs):
    used, padded = chunk
    others, out = refs[:-1], refs[-1]
    count = prefix.shape[0] // padded
    so_far = jnp.zeros((8, sums.shape[1]), F32)
    entering = jnp.zeros((padded, GW), F32)
    for n, other in enumerate(others):
        part = other[...].astype(F32)
        if n > 0:
            part = part * row_fades(groups, used, padded, where_ref[0], so_far, table)(0)
        entering += part
        so_far += dot(other[used : used + 8, :], unplace[...])[0:1]
    fade = row_fades(groups, used, padded, where_ref[0], sums[...], table)
    for k in range(count):
        part = slice(k * padded, (k + 1) * padded)
        out[part, :] = (prefix[part, :] + entering).astype(BF16)
        entering = fade(k) * entering


def project_kernel(groups, count, _, *refs):
    ins, (hin, gain, matrix, table, table_t) = refs[: 4 * count], refs[4 * count : 4 * count + 5]
    outs, (held, normed) = refs[4 * count + 5 : -2], refs[-2:]
    info, _ = group_rows(groups)
    share = ins[0].shape[0]

    @pl.when(pl.program_id(0) == 0)
    def _():
        for n in range(count):
            yl, qq, eR, gate = ins[4 * n : 4 * n + 4]
            reach = halves(eR[...])
            squares = jnp.zeros((share, table.shape[0]), F32)
            for g, (row, size, key) in enumerate(info):
                cols = slice(g * GW, (g + 1) * GW)
                outer = dot(qq[:, key : key + size], hin[row : row + size, :])
                y = yl[:, cols] + outer * dot2(reach, table[:, cols])
                gated = y * silu(gate[:, cols].astype(F32))
                held[:, cols] = gated
                squares += dot2(halves(gated * gated), table_t[cols, :])
            scale = halves(lax.rsqrt(squares * (1.0 / CH) + EPS))
            for g in range(groups):
                cols = slice(g * GW, (g + 1) * GW)
                unit = held[:, cols] * dot2(scale, table[:, cols]) * gain[:, cols].astype(F32)
                normed[n * share : (n + 1) * share, cols] = unit.astype(BF16)

    p = dot(normed[...], matrix[...]).astype(BF16)
    half = outs[0].shape[0]
    for n, out in enumerate(outs):
        out[...] = p[n * half : (n + 1) * half]


def place_kernel(unpick, back, out):
    out[...] = dot(unpick[...], back[...]).astype(BF16)


def norm_kernel(res, own, one, two, gain, after, x):
    total = own[...].astype(F32) + one[...].astype(F32) + two[...].astype(F32)
    mixed = (res[...].astype(F32) + total).astype(BF16)
    after[...] = mixed
    rows = mixed.astype(F32)
    scale = lax.rsqrt(jnp.mean(rows * rows, axis=1, keepdims=True) + EPS)
    x[...] = (rows * scale * gain[...].astype(F32)).astype(BF16)


def last_kernel(own_t, t1, t2, after_t, own_b, b1, b2, after_b, out):
    half = own_t.shape[0]
    for at, (own, one, two, after) in (
        (0, (own_t, t1, t2, after_t)),
        (half, (own_b, b1, b2, after_b)),
    ):
        total = own[...].astype(F32) + one[...].astype(F32) + two[...].astype(F32)
        out[at : at + half, :] = (after[...].astype(F32) + 0.5 * total).astype(BF16)


def pair_kernel(one, two, out):
    out[...] = (one[...].astype(F32) + two[...].astype(F32)).astype(BF16)


def feed_kernel(count, *refs):
    xs, (gate, up, down) = refs[:count], refs[count : count + 3]
    outs, total = refs[count + 3 : 2 * count + 3], refs[2 * count + 3]
    j = pl.program_id(0)
    x = jnp.concatenate([r[...] for r in xs], axis=0) if count > 1 else xs[0][...]
    hidden = (silu(dot(x, gate[...])) * dot(x, up[...])).astype(BF16)
    added = dot_nt(hidden, down[...])

    @pl.when(j == 0)
    def _():
        total[...] = added

    @pl.when(j > 0)
    def _():
        total[...] = total[...] + added

    @pl.when(j == pl.num_programs(0) - 1)
    def _():
        half = xs[0].shape[0]
        for n, out in enumerate(outs):
            out[...] = total[n * half : (n + 1) * half, :].astype(BF16)


def params(limit=VMEM_LIMIT):
    return pltpu.CompilerParams(dimension_semantics=("arbitrary",), vmem_limit_bytes=limit)


def cost(flops, moved):
    return pl.CostEstimate(flops=int(flops), bytes_accessed=int(moved), transcendentals=0)


def fixed(a):
    return pl.BlockSpec(a.shape, lambda *_: (0,) * a.ndim)


def whole(kernel, out_shapes, *args, flops=2e8):
    return pl.pallas_call(
        kernel,
        out_shape=out_shapes,
        compiler_params=pltpu.CompilerParams(vmem_limit_bytes=SMALL_LIMIT),
        cost_estimate=cost(flops, sum(a.size * 2 for a in args)),
    )(*args)


def ring(value, axis, step):
    count = lax.axis_size(axis)
    return lax.ppermute(value, axis, [(i, (i + step) % count) for i in range(count)])


def feed(xs, weights, tile=256):
    half, width = xs[0].shape
    inner = weights.shape[1] // 3
    tiles = inner // tile
    rows = half * len(xs)
    shape = jax.ShapeDtypeStruct((half, width), BF16)
    part = lambda n: pl.BlockSpec((width, tile), lambda j: (0, n * tiles + j))
    return pl.pallas_call(
        functools.partial(feed_kernel, len(xs)),
        grid=(tiles,),
        in_specs=[fixed(a) for a in xs] + [part(0), part(1), part(2)],
        out_specs=[pl.BlockSpec((half, width), lambda j: (0, 0))] * len(xs),
        out_shape=[shape] * len(xs),
        scratch_shapes=[pltpu.VMEM((rows, width), F32)],
        compiler_params=params(FEED_LIMIT),
        cost_estimate=cost(6 * rows * width * inner, weights.size * 2),
    )(*xs, weights, weights, weights)


def collect(own, left, right, opposite):
    send = lambda value, step: ring(value, "tp", step)
    from_left = send(opposite[0], 1)
    from_right = send(opposite[1], -1)
    bottom_left = send(right[1], 1)
    top_right = send(left[0], -1)
    shape = jax.ShapeDtypeStruct(own[0].shape, BF16)
    to_right = whole(pair_kernel, shape, right[0], from_left)
    to_left = whole(pair_kernel, shape, left[1], from_right)
    top_left = send(to_right, 1)
    bottom_right = send(to_left, -1)
    return (own[0], top_left, top_right), (own[1], bottom_left, bottom_right)


def on_device(
    residual, value_projected, gate_projected, wide_key_rows, wide_query_rows, narrow_key_rows,
    narrow_query_rows, step_before_softplus, extra_log_decay, log_decay_rate, value_kernel,
    wide_key_kernel, wide_query_kernel, narrow_key_kernel, narrow_query_kernel, head_norm_gain,
    output_matrix, feedforward_norm_gain, gate_matrix, up_matrix, down_matrix,
):
    sp, tp = lax.axis_size("sp"), lax.axis_size("tp")
    length, inner = value_projected.shape
    heads = inner // CH
    groups = heads // PER
    wcols, ncols = wide_key_rows.shape[1], narrow_key_rows.shape[1]
    keys = wcols + ncols
    width = output_matrix.shape[1]
    _, rows = group_rows(groups)
    near = 8 if sp % 8 == 0 else 2
    used = rows // near
    padded = -(-(used + 8) // 16) * 16
    chunk = (used, padded)
    blocks = length // BT
    me_sp, me_tp = lax.axis_index("sp"), lax.axis_index("tp")

    struct = jax.ShapeDtypeStruct
    table_np = (np.arange(heads)[:, None] == np.arange(inner)[None] // CH).astype(np.float32)
    table, table_t = jnp.asarray(table_np, BF16), jnp.asarray(table_np.T, BF16)
    place_np = np.zeros((heads, 2 * GW), np.float32)
    place_np[np.arange(heads), np.arange(heads)] = 1
    place_np[np.arange(heads), GW + heads + np.arange(heads)] = 1
    unplace_np = (place_np[:, :GW] + place_np[:, GW:]).T
    place, unplace = jnp.asarray(place_np, BF16), jnp.asarray(unplace_np, BF16)
    slot = np.arange(near * padded)
    pick_np = (
        (slot % padded < used)[:, None]
        & ((slot // padded * used + slot % padded)[:, None] == np.arange(rows)[None])
    ).astype(np.float32)
    pick, unpick = jnp.asarray(pick_np, BF16), jnp.asarray(pick_np.T, BF16)
    gather = jnp.asarray(
        (np.arange(near)[:, None] * padded + used == slot[None]).astype(np.float32), BF16
    )

    rowed = (
        value_projected, wide_key_rows, narrow_key_rows, wide_query_rows, narrow_query_rows
    )
    span = sum(a.shape[1] for a in rowed)
    mats = (gate_matrix, up_matrix, down_matrix)
    edge, weights = pl.pallas_call(
        edge_kernel,
        grid=(1,),
        in_specs=[
            pl.BlockSpec((EDGE, a.shape[1]), lambda i: (length // EDGE - 1, 0)) for a in rowed
        ]
        + [fixed(a) for a in mats],
        out_specs=[
            pl.BlockSpec((EDGE, span), lambda i: (0, 0)),
            pl.BlockSpec((mats[0].shape[0], 3 * mats[0].shape[1]), lambda i: (0, 0)),
        ],
        out_shape=[
            struct((EDGE, span), BF16),
            struct((mats[0].shape[0], 3 * mats[0].shape[1]), BF16),
        ],
        compiler_params=params(),
        cost_estimate=cost(1e6, 1e6),
    )(*rowed, *mats)
    rim = lax.ppermute(edge, "sp", [(i, i + 1) for i in range(sp - 1)])

    gain, ff_gain = head_norm_gain.reshape(1, inner), feedforward_norm_gain.reshape(1, width)
    rim, gain, ff_gain = lax.optimization_barrier((rim, gain, ff_gain))
    row_spec = lambda w: pl.BlockSpec((BT, w), lambda i: (i, 0))
    time_spec = pl.BlockSpec((heads, BT), lambda i: (0, i))
    rate = log_decay_rate.reshape(1, heads)
    up, kk, er, eR, hs, st = pl.pallas_call(
        functools.partial(states_kernel, groups, chunk),
        grid=(blocks,),
        in_specs=[
            fixed(rim), row_spec(inner), row_spec(wcols), row_spec(ncols), time_spec,
            time_spec, fixed(rate), fixed(value_kernel), fixed(wide_key_kernel),
            fixed(narrow_key_kernel), fixed(table), fixed(place), fixed(pick),
        ],
        out_specs=[
            row_spec(inner), row_spec(keys), row_spec(heads), row_spec(heads),
            pl.BlockSpec((1, rows, GW), lambda i: (i, 0, 0)),
            pl.BlockSpec((near * padded, GW), lambda i: (0, 0)),
        ],
        out_shape=[
            struct((length, inner), BF16), struct((length, keys), BF16),
            struct((length, heads), F32), struct((length, heads), F32),
            struct((blocks, rows, GW), BF16), struct((near * padded, GW), BF16),
        ],
        scratch_shapes=[
            pltpu.VMEM((EDGE + BT, inner), F32), pltpu.VMEM((EDGE + BT, keys), F32),
            pltpu.VMEM((rows, GW), F32), pltpu.VMEM((heads, BT), F32),
        ],
        compiler_params=params(),
        cost_estimate=cost(8e9, 6e6),
    )(
        rim, value_projected, wide_key_rows, narrow_key_rows, step_before_softplus.T,
        extra_log_decay.T, rate, value_kernel, wide_key_kernel, narrow_key_kernel, table, place,
        pick,
    )

    seats = [[q + n for n in range(near)] for q in range(0, sp, near)]
    exchange = lambda a: lax.all_to_all(a, "sp", 0, 0, axis_index_groups=seats, tiled=True)
    got = exchange(st)
    yl, qq = pl.pallas_call(
        functools.partial(inner_kernel, groups),
        grid=(blocks,),
        in_specs=[
            fixed(rim), row_spec(wcols), row_spec(ncols), fixed(wide_query_kernel),
            fixed(narrow_query_kernel), row_spec(keys), row_spec(inner), row_spec(heads),
            pl.BlockSpec((1, rows, GW), lambda i: (i, 0, 0)), fixed(table),
        ],
        out_specs=[row_spec(inner), row_spec(keys)],
        out_shape=[struct((length, inner), F32), struct((length, keys), BF16)],
        scratch_shapes=[pltpu.VMEM((EDGE + BT, keys), F32)],
        compiler_params=params(),
        cost_estimate=cost(8e9, 6e6),
    )(
        rim, wide_query_rows, narrow_query_rows, wide_query_kernel, narrow_query_kernel, kk, up,
        er, hs, table,
    )
    got, yl = lax.optimization_barrier((got, yl))
    far = [
        pltpu.with_memory_space_constraint(a, pltpu.HBM) for a in (yl, qq, eR, gate_projected, output_matrix)
    ]
    smem = pl.BlockSpec(memory_space=pltpu.SMEM)
    vmem = pl.BlockSpec(memory_space=pltpu.VMEM)
    seat = lax.rem(me_sp, near).reshape(1)
    prefix, sums, sent = pl.pallas_call(
        functools.partial(near_kernel, groups, chunk),
        in_specs=[smem] + [vmem] * 5,
        out_shape=[struct(st.shape, F32), struct((near, heads), F32), struct((padded, GW), BF16)],
        compiler_params=pltpu.CompilerParams(vmem_limit_bytes=SMALL_LIMIT),
        cost_estimate=cost(1e9, 1e6),
    )(seat, got, gather, unplace, place, table)
    others = [
        lax.ppermute(sent, "sp", [(i, i + near * n) for i in range(sp - near * n)])
        for n in range(1, sp // near)
    ]
    weights, *others = lax.optimization_barrier((weights, *others))
    weights = lax.all_gather(weights, "sp", axis=0, tiled=True)
    weights = pltpu.with_memory_space_constraint(weights, pltpu.HBM)
    entered = pl.pallas_call(
        functools.partial(far_kernel, groups, chunk),
        in_specs=[smem] + [vmem] * (4 + len(others)),
        out_shape=struct(st.shape, BF16),
        compiler_params=pltpu.CompilerParams(vmem_limit_bytes=SMALL_LIMIT),
        cost_estimate=cost(1e9, 1e6),
    )(seat, prefix, sums, unplace, table, *others)
    back = exchange(entered)
    hin = whole(place_kernel, struct((rows, GW), BF16), unpick, back)

    share = length // tp
    half = share // 2
    tile = 512

    def project(*offsets):
        count = len(offsets)
        mine = lambda w, n: pl.BlockSpec(
            (share, w), lambda i, me: (lax.rem(me[0] + offsets[n], tp), 0)
        )
        return pl.pallas_call(
            functools.partial(project_kernel, groups, count),
            grid_spec=pltpu.PrefetchScalarGridSpec(
                num_scalar_prefetch=1,
                grid=(width // tile,),
                in_specs=[mine(w, n) for n in range(count) for w in (inner, keys, heads, inner)]
                + [fixed(hin), fixed(gain), pl.BlockSpec((inner, tile), lambda i, o: (0, i))]
                + [fixed(table), fixed(table_t)],
                out_specs=[pl.BlockSpec((half, tile), lambda i, o: (0, i))] * (2 * count),
                scratch_shapes=[
                    pltpu.VMEM((share, inner), F32), pltpu.VMEM((count * share, inner), BF16)
                ],
            ),
            out_shape=[struct((half, width), BF16)] * (2 * count),
            compiler_params=params(FEED_LIMIT),
            cost_estimate=cost(2 * count * share * inner * width, 6e6),
        )(me_tp.reshape(1), *far[:4] * count, hin, gain, far[4], table, table_t)

    opposite, sides, own = project(2), project(1, 3), project(0)
    right, left = sides[:2], sides[2:]
    top, bottom = collect(own, left, right, opposite)
    pair = [struct((half, width), BF16)] * 2

    def norm(at, terms):
        same = pl.BlockSpec((half, width), lambda i: (0, 0))
        return pl.pallas_call(
            norm_kernel,
            grid=(1,),
            in_specs=[pl.BlockSpec((half, width), lambda i: (at, 0))]
            + [same] * 3
            + [fixed(ff_gain)],
            out_specs=[same] * 2,
            out_shape=pair,
            compiler_params=params(SMALL_LIMIT),
            cost_estimate=cost(1e9, 5 * half * width * 2),
        )(residual, *terms, ff_gain)

    (after_t, x_t), (after_b, x_b) = norm(0, top), norm(1, bottom)

    left_t, right_b = ring(x_t, "tp", 1), ring(x_b, "tp", -1)
    left_b, right_t = ring(x_b, "tp", 1), ring(x_t, "tp", -1)
    opp_t, opp_b = ring(left_t, "tp", 1), ring(right_b, "tp", -1)
    own = feed([x_t, x_b], weights)
    near = feed([left_t, left_b, right_t, right_b], weights)
    opposite = feed([opp_t, opp_b], weights)
    top, bottom = collect(own, near[:2], near[2:], opposite)
    return whole(
        last_kernel, struct((share, width), BF16), *top, after_t, *bottom, after_b
    )


def solution(mesh):
    rows = P(("grp", "sp"), "tp")
    in_specs = (P(("grp", "sp", "tp"), None),) + (rows,) * 8 + (P("tp"),) + (P(None, "tp"),) * 5
    in_specs += (P("tp"), P("tp", None), P()) + (P("sp", "tp"),) * 3
    return jax.shard_map(
        on_device,
        mesh=mesh,
        in_specs=in_specs,
        out_specs=P(("grp", "sp", "tp"), None),
        check_vma=False,
    )
```

```python
import functools

import jax
import jax.numpy as jnp
import numpy as np
from jax import lax
from jax.experimental import pallas as pl
from jax.experimental.pallas import tpu as pltpu
from jax.sharding import PartitionSpec as P


CH = 64
PER = 4
GW = PER * CH
BT = 128
WIDE = 128
NARROW = 64
TAPS = 4
LANES = 128
STRIP = 32
EDGE = 8
EPS = 1e-6
F32 = jnp.float32
BF16 = jnp.bfloat16
VMEM_LIMIT = 60 << 20
SMALL_LIMIT = 12 << 20
FEED_LIMIT = 24 << 20


def dot(a, b):
    return jnp.dot(a, b, preferred_element_type=F32)


def dot_nt(a, b):
    return lax.dot_general(a, b, (((1,), (1,)), ((), ())), preferred_element_type=F32)


def dot_tn(a, b):
    return lax.dot_general(a, b, (((0,), (0,)), ((), ())), preferred_element_type=F32)


def halves(x):
    hi = x.astype(BF16)
    return hi, (x - hi.astype(F32)).astype(BF16)


def dot2(pair, b):
    return dot(pair[0], b) + dot(pair[1], b)


def stacked_columns(x):
    hi = x.astype(BF16).astype(F32)
    return jnp.concatenate([hi, x - hi], axis=0).T.astype(BF16)


def silu(x):
    h = 0.5 * x
    return h + h * jnp.tanh(h)


def group_rows(groups):
    out, row = [], 0
    wide_cols = (groups // 2) * WIDE
    for g in range(groups):
        size = NARROW if g % 2 else WIDE
        key = wide_cols + (g // 2) * NARROW if g % 2 else (g // 2) * WIDE
        out.append((row, size, key))
        row += size
    return out, row


def fill(buf, rows, x):
    for n in range(x.shape[1] // LANES):
        buf[n, rows, :] = x[:, n * LANES : (n + 1) * LANES].astype(F32)


def conv_plane(buf, plane, ker, row):
    k = ker.astype(F32)
    first = row + EDGE - TAPS + 1
    total = buf[plane, first : first + STRIP, :] * k[0:1]
    for tap in range(1, TAPS):
        total += buf[plane, first + tap : first + tap + STRIP, :] * k[tap : tap + 1]
    return silu(total).astype(BF16)


def conv_all(buf, kernels, out):
    plane = 0
    for ker in kernels:
        for c in range(0, ker.shape[1], LANES):
            cols = slice(plane * LANES, (plane + 1) * LANES)
            for row in range(0, BT, STRIP):
                out[row : row + STRIP, cols] = conv_plane(buf, plane, ker[:, c : c + LANES], row)
            plane += 1


def join_kernel(*refs):
    at = 0
    for part in refs[:-1]:
        refs[-1][:, at : at + part.shape[1]] = part[...]
        at += part.shape[1]


def states_kernel(
    groups, chunk, rim, value, wk, nk, step, extra, rate, kv, kwk, knk, table, place, pick,
    up, kk, er, eR, hs, st, bufv, bufk, state, before,
):
    i = pl.program_id(0)
    info, _ = group_rows(groups)
    inner, wcols, ncols = value.shape[1], wk.shape[1], nk.shape[1]

    @pl.when(i == 0)
    def _():
        fill(bufv, slice(0, EDGE), rim[:, 0:inner])
        fill(bufk, slice(0, EDGE), rim[:, inner : inner + wcols + ncols])
        state[...] = jnp.zeros_like(state)
        before[...] = jnp.zeros_like(before)

    body = slice(EDGE, EDGE + BT)
    fill(bufv, body, value)
    fill(bufk, body, wk)
    fill(bufk.at[wcols // LANES :], body, nk)

    heads = step.shape[0]
    diagonal = lax.broadcasted_iota(jnp.int32, (heads, heads), 0) == lax.broadcasted_iota(
        jnp.int32, (heads, heads), 1
    )
    speed = jnp.exp(jnp.sum(jnp.where(diagonal, rate[...], 0.0), axis=1, keepdims=True))
    dt = jnp.log(1.0 + jnp.exp(step[...]))
    a = extra[...] - speed * dt
    upto = lax.broadcasted_iota(jnp.int32, (BT, BT), 0) <= lax.broadcasted_iota(
        jnp.int32, (BT, BT), 1
    )
    upto = jnp.where(upto, 1.0, 0.0).astype(BF16)
    a1 = a.astype(BF16)
    a2, a3 = halves(a - a1.astype(F32))
    r = dot(a1, upto) + dot(a2, upto) + dot(a3, upto)
    mid, end = r[:, BT // 2 - 1 : BT // 2], r[:, BT - 1 : BT]
    er[...] = stacked_columns(jnp.exp(r - mid))
    eR[...] = stacked_columns(jnp.exp(r + before[...]))
    before[...] = before[...] + end
    inward = stacked_columns(jnp.exp(mid - r) * dt)
    lane = lax.broadcasted_iota(jnp.int32, r.shape, 1)
    scales = jnp.exp(jnp.where(lane == 0, mid, jnp.where(lane == 1, end, end - mid)))
    scales = stacked_columns(scales)[0:16]

    conv_all(bufk, (kwk, knk), kk)
    for g, (row, size, key) in enumerate(info):
        cols = slice(g * GW, (g + 1) * GW)
        tab = table[:, cols]
        f = dot(inward, tab)
        s = dot(scales, tab)
        for n in range(GW // LANES):
            plane = g * (GW // LANES) + n
            part = slice(plane * LANES, (plane + 1) * LANES)
            for at in range(0, BT, STRIP):
                strip = slice(at, at + STRIP)
                u = conv_plane(bufv, plane, kv[:, part], at).astype(F32)
                up[strip, part] = (u * f[strip, n * LANES : (n + 1) * LANES]).astype(BF16)
        scaled = up[:, cols]
        added = dot_tn(kk[:, key : key + size], scaled)
        old = state[row : row + size, :]
        hs[0, row : row + size, :] = (old * s[0:1]).astype(BF16)
        state[row : row + size, :] = old * s[1:2] + added * s[2:3]
    bufv[:, 0:EDGE, :] = bufv[:, BT:, :]
    bufk[:, 0:EDGE, :] = bufk[:, BT:, :]

    @pl.when(i == pl.num_programs(0) - 1)
    def _():
        total = halves(before[...].T[0:8])
        line_t = (dot(total[0], place[:, 0:GW]) + dot(total[1], place[:, GW:]))[0:1]
        sent = dot(pick[...], state[...].astype(BF16))
        used, padded = chunk
        rows = lax.broadcasted_iota(jnp.int32, sent.shape, 0)
        st[...] = jnp.where(rows % padded == used, line_t, sent).astype(BF16)


def inner_kernel(groups, rim, wq, nq, kwq, knq, kk, up, er, hs, table, yl, qq, bufq):
    i = pl.program_id(0)
    info, _ = group_rows(groups)
    wcols, ncols = wq.shape[1], nq.shape[1]

    @pl.when(i == 0)
    def _():
        fill(bufq, slice(0, EDGE), rim[:, rim.shape[1] - wcols - ncols :])

    body = slice(EDGE, EDGE + BT)
    fill(bufq, body, wq)
    fill(bufq.at[wcols // LANES :], body, nq)
    conv_all(bufq, (kwq, knq), qq)
    bufq[:, 0:EDGE, :] = bufq[:, BT:, :]
    outward = er[...]
    t = lax.broadcasted_iota(jnp.int32, (BT, BT), 0)
    s = lax.broadcasted_iota(jnp.int32, (BT, BT), 1)
    for g, (row, size, key) in enumerate(info):
        cols = slice(g * GW, (g + 1) * GW)
        q, k = qq[:, key : key + size], kk[:, key : key + size]
        weights = jnp.where(s <= t, dot_nt(q, k), 0.0).astype(BF16)
        y = dot(weights, up[:, cols]) + dot(q, hs[0, row : row + size, :])
        yl[:, cols] = y * dot(outward, table[:, cols])


def row_fades(groups, used, padded, place, sums, table):
    info, _ = group_rows(groups)
    factor = halves(jnp.exp(sums))
    heads = table.shape[0] // 2
    fades = [dot2(factor, table[:heads, g * GW : (g + 1) * GW]) for g in range(groups)]
    row = lax.broadcasted_iota(jnp.int32, (padded, GW), 0) + place * used
    masks = [row >= info[g][0] for g in range(1, groups)]

    def fade(k):
        out = jnp.broadcast_to(fades[0][k : k + 1], (padded, GW))
        for g in range(1, groups):
            out = jnp.where(masks[g - 1], fades[g][k : k + 1], out)
        return out

    return fade


def near_kernel(groups, chunk, where_ref, got, gather, unplace, place, table, prefix, sums, sent):
    used, padded = chunk
    count = got.shape[0] // padded
    lines = dot(gather[...], got[...]).astype(BF16)
    logs = dot(lines, unplace[...])
    sums[...] = logs
    fade = row_fades(groups, used, padded, where_ref[0], logs, table)
    held = jnp.zeros((padded, GW), F32)
    for k in range(count):
        part = slice(k * padded, (k + 1) * padded)
        prefix[part, :] = held
        held = fade(k) * held + got[part, :].astype(F32)
    total = halves(jnp.broadcast_to(jnp.sum(logs, axis=0, keepdims=True), (8, logs.shape[1])))
    line = (dot(total[0], place[:, 0:GW]) + dot(total[1], place[:, GW:]))[0:1]
    row = lax.broadcasted_iota(jnp.int32, held.shape, 0)
    sent[...] = jnp.where(row == used, line, held).astype(BF16)


def far_kernel(groups, chunk, where_ref, prefix, sums, unplace, table, *refs):
    used, padded = chunk
    others, out = refs[:-1], refs[-1]
    count = prefix.shape[0] // padded
    so_far = jnp.zeros((8, sums.shape[1]), F32)
    entering = jnp.zeros((padded, GW), F32)
    for n, other in enumerate(others):
        part = other[...].astype(F32)
        if n > 0:
            part = part * row_fades(groups, used, padded, where_ref[0], so_far, table)(0)
        entering += part
        so_far += dot(other[used : used + 8, :], unplace[...])[0:1]
    fade = row_fades(groups, used, padded, where_ref[0], sums[...], table)
    for k in range(count):
        part = slice(k * padded, (k + 1) * padded)
        out[part, :] = (prefix[part, :] + entering).astype(BF16)
        entering = fade(k) * entering


def project_kernel(groups, count, _, *refs):
    ins, (hin, gain, matrix, table, table_t) = refs[: 4 * count], refs[4 * count : 4 * count + 5]
    outs, (held, normed) = refs[4 * count + 5 : -2], refs[-2:]
    info, _ = group_rows(groups)
    share = ins[0].shape[0]

    @pl.when(pl.program_id(0) == 0)
    def _():
        for n in range(count):
            yl, qq, eR, gate = ins[4 * n : 4 * n + 4]
            reach = eR[...]
            squares = jnp.zeros((share, table.shape[0] // 2), F32)
            for g, (row, size, key) in enumerate(info):
                cols = slice(g * GW, (g + 1) * GW)
                outer = dot(qq[:, key : key + size], hin[row : row + size, :])
                y = yl[:, cols] + outer * dot(reach, table[:, cols])
                gated = y * silu(gate[:, cols].astype(F32))
                held[:, cols] = gated
                squares += dot2(halves(gated * gated), table_t[cols, :])
            scale = halves(lax.rsqrt(squares * (1.0 / CH) + EPS))
            for g in range(groups):
                cols = slice(g * GW, (g + 1) * GW)
                unit = held[:, cols] * dot2(scale, table[: table.shape[0] // 2, cols]) * gain[:, cols].astype(F32)
                normed[n * share : (n + 1) * share, cols] = unit.astype(BF16)

    p = dot(normed[...], matrix[...]).astype(BF16)
    half = outs[0].shape[0]
    for n, out in enumerate(outs):
        out[...] = p[n * half : (n + 1) * half]


def place_kernel(unpick, back, out):
    out[...] = dot(unpick[...], back[...]).astype(BF16)


def norm_kernel(res, own, one, two, gain, after, x):
    total = own[...].astype(F32) + one[...].astype(F32) + two[...].astype(F32)
    mixed = (res[...].astype(F32) + total).astype(BF16)
    after[...] = mixed
    rows = mixed.astype(F32)
    scale = lax.rsqrt(jnp.mean(rows * rows, axis=1, keepdims=True) + EPS)
    x[...] = (rows * scale * gain[...].astype(F32)).astype(BF16)


def last_kernel(own_t, t1, t2, after_t, own_b, b1, b2, after_b, out):
    half = own_t.shape[0]
    for at, (own, one, two, after) in (
        (0, (own_t, t1, t2, after_t)),
        (half, (own_b, b1, b2, after_b)),
    ):
        total = own[...].astype(F32) + one[...].astype(F32) + two[...].astype(F32)
        out[at : at + half, :] = (after[...].astype(F32) + 0.5 * total).astype(BF16)


def pair_kernel(one, two, out):
    out[...] = (one[...].astype(F32) + two[...].astype(F32)).astype(BF16)


def feed_kernel(count, *refs):
    xs, (gate, up, down) = refs[:count], refs[count : count + 3]
    outs, total = refs[count + 3 : 2 * count + 3], refs[2 * count + 3]
    j = pl.program_id(0)
    x = jnp.concatenate([r[...] for r in xs], axis=0) if count > 1 else xs[0][...]
    hidden = (silu(dot(x, gate[...])) * dot(x, up[...])).astype(BF16)
    added = dot_nt(hidden, down[...])

    @pl.when(j == 0)
    def _():
        total[...] = added

    @pl.when(j > 0)
    def _():
        total[...] = total[...] + added

    @pl.when(j == pl.num_programs(0) - 1)
    def _():
        half = xs[0].shape[0]
        for n, out in enumerate(outs):
            out[...] = total[n * half : (n + 1) * half, :].astype(BF16)


def params(limit=VMEM_LIMIT):
    return pltpu.CompilerParams(dimension_semantics=("arbitrary",), vmem_limit_bytes=limit)


def cost(flops, moved):
    return pl.CostEstimate(flops=int(flops), bytes_accessed=int(moved), transcendentals=0)


def fixed(a):
    return pl.BlockSpec(a.shape, lambda *_: (0,) * a.ndim)


def whole(kernel, out_shapes, *args, flops=2e8):
    return pl.pallas_call(
        kernel,
        out_shape=out_shapes,
        compiler_params=pltpu.CompilerParams(vmem_limit_bytes=SMALL_LIMIT),
        cost_estimate=cost(flops, sum(a.size * 2 for a in args)),
    )(*args)


def ring(value, axis, step):
    count = lax.axis_size(axis)
    return lax.ppermute(value, axis, [(i, (i + step) % count) for i in range(count)])


def feed(xs, weights, tile=256):
    half, width = xs[0].shape
    inner = weights.shape[1] // 3
    tiles = inner // tile
    rows = half * len(xs)
    shape = jax.ShapeDtypeStruct((half, width), BF16)
    part = lambda n: pl.BlockSpec((width, tile), lambda j: (0, n * tiles + j))
    return pl.pallas_call(
        functools.partial(feed_kernel, len(xs)),
        grid=(tiles,),
        in_specs=[fixed(a) for a in xs] + [part(0), part(1), part(2)],
        out_specs=[pl.BlockSpec((half, width), lambda j: (0, 0))] * len(xs),
        out_shape=[shape] * len(xs),
        scratch_shapes=[pltpu.VMEM((rows, width), F32)],
        compiler_params=params(FEED_LIMIT),
        cost_estimate=cost(6 * rows * width * inner, weights.size * 2),
    )(*xs, weights, weights, weights)


def collect(own, left, right, opposite):
    send = lambda value, step: ring(value, "tp", step)
    from_left = send(opposite[0], 1)
    from_right = send(opposite[1], -1)
    bottom_left = send(right[1], 1)
    top_right = send(left[0], -1)
    shape = jax.ShapeDtypeStruct(own[0].shape, BF16)
    to_right = whole(pair_kernel, shape, right[0], from_left)
    to_left = whole(pair_kernel, shape, left[1], from_right)
    top_left = send(to_right, 1)
    bottom_right = send(to_left, -1)
    return (own[0], top_left, top_right), (own[1], bottom_left, bottom_right)


def on_device(
    residual, value_projected, gate_projected, wide_key_rows, wide_query_rows, narrow_key_rows,
    narrow_query_rows, step_before_softplus, extra_log_decay, log_decay_rate, value_kernel,
    wide_key_kernel, wide_query_kernel, narrow_key_kernel, narrow_query_kernel, head_norm_gain,
    output_matrix, feedforward_norm_gain, gate_matrix, up_matrix, down_matrix,
):
    sp, tp = lax.axis_size("sp"), lax.axis_size("tp")
    length, inner = value_projected.shape
    heads = inner // CH
    groups = heads // PER
    wcols, ncols = wide_key_rows.shape[1], narrow_key_rows.shape[1]
    keys = wcols + ncols
    width = output_matrix.shape[1]
    _, rows = group_rows(groups)
    near = 8 if sp % 8 == 0 else 2
    used = rows // near
    padded = -(-(used + 8) // 16) * 16
    chunk = (used, padded)
    blocks = length // BT
    me_sp, me_tp = lax.axis_index("sp"), lax.axis_index("tp")

    struct = jax.ShapeDtypeStruct
    table_np = (np.arange(heads)[:, None] == np.arange(inner)[None] // CH).astype(np.float32)
    table = jnp.asarray(np.concatenate([table_np, table_np]), BF16)
    table_t = jnp.asarray(table_np.T, BF16)
    place_np = np.zeros((heads, 2 * GW), np.float32)
    place_np[np.arange(heads), np.arange(heads)] = 1
    place_np[np.arange(heads), GW + heads + np.arange(heads)] = 1
    unplace_np = (place_np[:, :GW] + place_np[:, GW:]).T
    place, unplace = jnp.asarray(place_np, BF16), jnp.asarray(unplace_np, BF16)
    slot = np.arange(near * padded)
    pick_np = (
        (slot % padded < used)[:, None]
        & ((slot // padded * used + slot % padded)[:, None] == np.arange(rows)[None])
    ).astype(np.float32)
    pick, unpick = jnp.asarray(pick_np, BF16), jnp.asarray(pick_np.T, BF16)
    gather = jnp.asarray(
        (np.arange(near)[:, None] * padded + used == slot[None]).astype(np.float32), BF16
    )

    rowed = (
        value_projected, wide_key_rows, narrow_key_rows, wide_query_rows, narrow_query_rows
    )

    def joined(arrays, specs):
        shape = (specs[0].block_shape[0], sum(a.shape[1] for a in arrays))
        return pl.pallas_call(
            join_kernel,
            grid=(1,),
            in_specs=specs,
            out_specs=pl.BlockSpec(shape, lambda i: (0, 0)),
            out_shape=struct(shape, BF16),
            compiler_params=params(),
            cost_estimate=cost(1e6, 1e6),
        )(*arrays)

    ends = [pl.BlockSpec((EDGE, a.shape[1]), lambda i: (length // EDGE - 1, 0)) for a in rowed]
    edge = joined(rowed, ends)
    rim = lax.ppermute(edge, "sp", [(i, i + 1) for i in range(sp - 1)])

    mats = (gate_matrix, up_matrix, down_matrix)
    weights = joined(mats, [fixed(a) for a in mats])
    gain, ff_gain = head_norm_gain.reshape(1, inner), feedforward_norm_gain.reshape(1, width)
    rim, gain, ff_gain, weights = lax.optimization_barrier((rim, gain, ff_gain, weights))
    rim = pltpu.with_memory_space_constraint(rim, pltpu.HBM)
    row_spec = lambda w: pl.BlockSpec((BT, w), lambda i: (i, 0))
    planes = lambda w: pltpu.VMEM((w // LANES, EDGE + BT, LANES), F32)
    time_spec = pl.BlockSpec((heads, BT), lambda i: (0, i))
    rate = log_decay_rate.reshape(1, heads)
    up, kk, er, eR, hs, st = pl.pallas_call(
        functools.partial(states_kernel, groups, chunk),
        grid=(blocks,),
        in_specs=[
            fixed(rim), row_spec(inner), row_spec(wcols), row_spec(ncols), time_spec,
            time_spec, fixed(rate), fixed(value_kernel), fixed(wide_key_kernel),
            fixed(narrow_key_kernel), fixed(table), fixed(place), fixed(pick),
        ],
        out_specs=[
            row_spec(inner), row_spec(keys), row_spec(2 * heads), row_spec(2 * heads),
            pl.BlockSpec((1, rows, GW), lambda i: (i, 0, 0)),
            pl.BlockSpec((near * padded, GW), lambda i: (0, 0)),
        ],
        out_shape=[
            struct((length, inner), BF16), struct((length, keys), BF16),
            struct((length, 2 * heads), BF16), struct((length, 2 * heads), BF16),
            struct((blocks, rows, GW), BF16), struct((near * padded, GW), BF16),
        ],
        scratch_shapes=[
            planes(inner), planes(keys),
            pltpu.VMEM((rows, GW), F32), pltpu.VMEM((heads, BT), F32),
        ],
        compiler_params=params(),
        cost_estimate=cost(8e9, 6e6),
    )(
        rim, value_projected, wide_key_rows, narrow_key_rows, step_before_softplus.T,
        extra_log_decay.T, rate, value_kernel, wide_key_kernel, narrow_key_kernel, table, place,
        pick,
    )

    weights, st = lax.optimization_barrier((weights, st))
    weights = lax.all_gather(weights, "sp", axis=0, tiled=True)
    weights = pltpu.with_memory_space_constraint(weights, pltpu.HBM)
    seats = [[q + n for n in range(near)] for q in range(0, sp, near)]
    exchange = lambda a: lax.all_to_all(a, "sp", 0, 0, axis_index_groups=seats, tiled=True)
    got = exchange(st)
    inner_call = pl.pallas_call(
        functools.partial(inner_kernel, groups),
        grid=(blocks,),
        in_specs=[
            fixed(rim), row_spec(wcols), row_spec(ncols), fixed(wide_query_kernel),
            fixed(narrow_query_kernel), row_spec(keys), row_spec(inner), row_spec(2 * heads),
            pl.BlockSpec((1, rows, GW), lambda i: (i, 0, 0)), fixed(table),
        ],
        out_specs=[row_spec(inner), row_spec(keys)],
        out_shape=[struct((length, inner), F32), struct((length, keys), BF16)],
        scratch_shapes=[planes(keys)],
        compiler_params=params(),
        cost_estimate=cost(8e9, 6e6),
    )
    smem = pl.BlockSpec(memory_space=pltpu.SMEM)
    vmem = pl.BlockSpec(memory_space=pltpu.VMEM)
    seat = lax.rem(me_sp, near).reshape(1)
    prefix, sums, sent = pl.pallas_call(
        functools.partial(near_kernel, groups, chunk),
        in_specs=[smem] + [vmem] * 5,
        out_shape=[struct(st.shape, F32), struct((near, heads), F32), struct((padded, GW), BF16)],
        compiler_params=pltpu.CompilerParams(vmem_limit_bytes=SMALL_LIMIT),
        cost_estimate=cost(1e9, 1e6),
    )(seat, got, gather, unplace, place, table)
    others = [
        lax.ppermute(sent, "sp", [(i, i + near * n) for i in range(sp - near * n)])
        for n in range(1, sp // near)
    ]
    entered = pl.pallas_call(
        functools.partial(far_kernel, groups, chunk),
        in_specs=[smem] + [vmem] * (4 + len(others)),
        out_shape=struct(st.shape, BF16),
        compiler_params=pltpu.CompilerParams(vmem_limit_bytes=SMALL_LIMIT),
        cost_estimate=cost(1e9, 1e6),
    )(seat, prefix, sums, unplace, table, *others)
    er, entered = lax.optimization_barrier((er, entered))
    back = exchange(entered)
    yl, qq = inner_call(
        rim, wide_query_rows, narrow_query_rows, wide_query_kernel, narrow_query_kernel, kk, up,
        er, hs, table,
    )
    far = [
        pltpu.with_memory_space_constraint(a, pltpu.HBM) for a in (yl, qq, eR, gate_projected, output_matrix)
    ]
    hin = whole(place_kernel, struct((rows, GW), BF16), unpick, back)

    share = length // tp
    half = share // 2
    tile = 512

    def project(*offsets):
        count = len(offsets)
        mine = lambda w, n: pl.BlockSpec(
            (share, w), lambda i, me: (lax.rem(me[0] + offsets[n], tp), 0)
        )
        return pl.pallas_call(
            functools.partial(project_kernel, groups, count),
            grid_spec=pltpu.PrefetchScalarGridSpec(
                num_scalar_prefetch=1,
                grid=(width // tile,),
                in_specs=[mine(w, n) for n in range(count) for w in (inner, keys, 2 * heads, inner)]
                + [fixed(hin), fixed(gain), pl.BlockSpec((inner, tile), lambda i, o: (0, i))]
                + [fixed(table), fixed(table_t)],
                out_specs=[pl.BlockSpec((half, tile), lambda i, o: (0, i))] * (2 * count),
                scratch_shapes=[
                    pltpu.VMEM((share, inner), F32), pltpu.VMEM((count * share, inner), BF16)
                ],
            ),
            out_shape=[struct((half, width), BF16)] * (2 * count),
            compiler_params=params(FEED_LIMIT),
            cost_estimate=cost(2 * count * share * inner * width, 6e6),
        )(me_tp.reshape(1), *far[:4] * count, hin, gain, far[4], table, table_t)

    opposite, sides, own = project(2), project(1, 3), project(0)
    right, left = sides[:2], sides[2:]
    top, bottom = collect(own, left, right, opposite)
    pair = [struct((half, width), BF16)] * 2

    def norm(at, terms):
        same = pl.BlockSpec((half, width), lambda i: (0, 0))
        return pl.pallas_call(
            norm_kernel,
            grid=(1,),
            in_specs=[pl.BlockSpec((half, width), lambda i: (at, 0))]
            + [same] * 3
            + [fixed(ff_gain)],
            out_specs=[same] * 2,
            out_shape=pair,
            compiler_params=params(SMALL_LIMIT),
            cost_estimate=cost(1e9, 5 * half * width * 2),
        )(residual, *terms, ff_gain)

    (after_t, x_t), (after_b, x_b) = norm(0, top), norm(1, bottom)

    left_t, right_b = ring(x_t, "tp", 1), ring(x_b, "tp", -1)
    left_b, right_t = ring(x_b, "tp", 1), ring(x_t, "tp", -1)
    opp_t, opp_b = ring(left_t, "tp", 1), ring(right_b, "tp", -1)
    own = feed([x_t, x_b], weights)
    near = feed([left_t, left_b, right_t, right_b], weights)
    opposite = feed([opp_t, opp_b], weights)
    top, bottom = collect(own, near[:2], near[2:], opposite)
    return whole(
        last_kernel, struct((share, width), BF16), *top, after_t, *bottom, after_b
    )


def solution(mesh):
    rows = P(("grp", "sp"), "tp")
    in_specs = (P(("grp", "sp", "tp"), None),) + (rows,) * 8 + (P("tp"),) + (P(None, "tp"),) * 5
    in_specs += (P("tp"), P("tp", None), P()) + (P("sp", "tp"),) * 3
    return jax.shard_map(
        on_device,
        mesh=mesh,
        in_specs=in_specs,
        out_specs=P(("grp", "sp", "tp"), None),
        check_vma=False,
    )
```

```python
import functools

import jax
import jax.numpy as jnp
import numpy as np
from jax import lax
from jax.experimental import pallas as pl
from jax.experimental.pallas import tpu as pltpu
from jax.sharding import PartitionSpec as P


CH = 64
PER = 4
GW = PER * CH
BT = 128
WIDE = 128
NARROW = 64
TAPS = 4
LANES = 128
STRIP = 32
EDGE = 8
EPS = 1e-6
F32 = jnp.float32
BF16 = jnp.bfloat16
VMEM_LIMIT = 60 << 20
SMALL_LIMIT = 12 << 20
FEED_LIMIT = 24 << 20


def dot(a, b):
    return jnp.dot(a, b, preferred_element_type=F32)


def dot_nt(a, b):
    return lax.dot_general(a, b, (((1,), (1,)), ((), ())), preferred_element_type=F32)


def dot_tn(a, b):
    return lax.dot_general(a, b, (((0,), (0,)), ((), ())), preferred_element_type=F32)


def halves(x):
    hi = x.astype(BF16)
    return hi, (x - hi.astype(F32)).astype(BF16)


def dot2(pair, b):
    return dot(pair[0], b) + dot(pair[1], b)


def stacked_columns(x):
    hi = x.astype(BF16).astype(F32)
    return jnp.concatenate([hi, x - hi], axis=0).T.astype(BF16)


def silu(x):
    h = 0.5 * x
    return h + h * jnp.tanh(h)


def group_rows(groups):
    out, row = [], 0
    wide_cols = (groups // 2) * WIDE
    for g in range(groups):
        size = NARROW if g % 2 else WIDE
        key = wide_cols + (g // 2) * NARROW if g % 2 else (g // 2) * WIDE
        out.append((row, size, key))
        row += size
    return out, row


def fill(buf, rows, x):
    for n in range(x.shape[1] // LANES):
        buf[n, rows, :] = x[:, n * LANES : (n + 1) * LANES].astype(F32)


def conv_plane(buf, plane, ker, row):
    k = ker.astype(F32)
    first = row + EDGE - TAPS + 1
    total = buf[plane, first : first + STRIP, :] * k[0:1]
    for tap in range(1, TAPS):
        total += buf[plane, first + tap : first + tap + STRIP, :] * k[tap : tap + 1]
    return silu(total).astype(BF16)


def conv_all(buf, kernels, out):
    plane = 0
    for ker in kernels:
        for c in range(0, ker.shape[1], LANES):
            cols = slice(plane * LANES, (plane + 1) * LANES)
            for row in range(0, BT, STRIP):
                out[row : row + STRIP, cols] = conv_plane(buf, plane, ker[:, c : c + LANES], row)
            plane += 1


def join_kernel(*refs):
    at = 0
    for part in refs[:-1]:
        refs[-1][:, at : at + part.shape[1]] = part[...]
        at += part.shape[1]


def states_kernel(
    groups, chunk, rim, value, wk, nk, step, extra, rate, kv, kwk, knk, table, place, pick,
    up, kk, er, eR, hs, st, bufv, bufk, state, before,
):
    i = pl.program_id(0)
    info, _ = group_rows(groups)
    inner, wcols, ncols = value.shape[1], wk.shape[1], nk.shape[1]

    @pl.when(i == 0)
    def _():
        fill(bufv, slice(0, EDGE), rim[:, 0:inner])
        fill(bufk, slice(0, EDGE), rim[:, inner : inner + wcols + ncols])
        state[...] = jnp.zeros_like(state)
        before[...] = jnp.zeros_like(before)

    body = slice(EDGE, EDGE + BT)
    fill(bufv, body, value)
    fill(bufk, body, wk)
    fill(bufk.at[wcols // LANES :], body, nk)

    heads = step.shape[0]
    diagonal = lax.broadcasted_iota(jnp.int32, (heads, heads), 0) == lax.broadcasted_iota(
        jnp.int32, (heads, heads), 1
    )
    speed = jnp.exp(jnp.sum(jnp.where(diagonal, rate[...], 0.0), axis=1, keepdims=True))
    dt = jnp.log(1.0 + jnp.exp(step[...]))
    a = extra[...] - speed * dt
    upto = lax.broadcasted_iota(jnp.int32, (BT, BT), 0) <= lax.broadcasted_iota(
        jnp.int32, (BT, BT), 1
    )
    upto = jnp.where(upto, 1.0, 0.0).astype(BF16)
    a1 = a.astype(BF16)
    a2, a3 = halves(a - a1.astype(F32))
    r = dot(a1, upto) + dot(a2, upto) + dot(a3, upto)
    mid, end = r[:, BT // 2 - 1 : BT // 2], r[:, BT - 1 : BT]
    er[...] = stacked_columns(jnp.exp(r - mid))
    eR[...] = stacked_columns(jnp.exp(r + before[...]))
    before[...] = before[...] + end
    inward = stacked_columns(jnp.exp(mid - r) * dt)
    lane = lax.broadcasted_iota(jnp.int32, r.shape, 1)
    scales = jnp.exp(jnp.where(lane == 0, mid, jnp.where(lane == 1, end, end - mid)))
    scales = stacked_columns(scales)[0:16]

    conv_all(bufk, (kwk, knk), kk)
    for g, (row, size, key) in enumerate(info):
        cols = slice(g * GW, (g + 1) * GW)
        tab = table[:, cols]
        f = dot(inward, tab)
        s = dot(scales, tab)
        for n in range(GW // LANES):
            plane = g * (GW // LANES) + n
            part = slice(plane * LANES, (plane + 1) * LANES)
            for at in range(0, BT, STRIP):
                strip = slice(at, at + STRIP)
                u = conv_plane(bufv, plane, kv[:, part], at).astype(F32)
                up[strip, part] = (u * f[strip, n * LANES : (n + 1) * LANES]).astype(BF16)
        scaled = up[:, cols]
        added = dot_tn(kk[:, key : key + size], scaled)
        old = state[row : row + size, :]
        hs[0, row : row + size, :] = (old * s[0:1]).astype(BF16)
        state[row : row + size, :] = old * s[1:2] + added * s[2:3]
    bufv[:, 0:EDGE, :] = bufv[:, BT:, :]
    bufk[:, 0:EDGE, :] = bufk[:, BT:, :]

    @pl.when(i == pl.num_programs(0) - 1)
    def _():
        total = halves(before[...].T[0:8])
        line_t = (dot(total[0], place[:, 0:GW]) + dot(total[1], place[:, GW:]))[0:1]
        sent = dot(pick[...], state[...].astype(BF16))
        used, padded = chunk
        rows = lax.broadcasted_iota(jnp.int32, sent.shape, 0)
        st[...] = jnp.where(rows % padded == used, line_t, sent).astype(BF16)


def inner_kernel(groups, rim, wq, nq, kwq, knq, kk, up, er, hs, table, yl, qq, bufq):
    i = pl.program_id(0)
    info, _ = group_rows(groups)
    wcols, ncols = wq.shape[1], nq.shape[1]

    @pl.when(i == 0)
    def _():
        fill(bufq, slice(0, EDGE), rim[:, rim.shape[1] - wcols - ncols :])

    body = slice(EDGE, EDGE + BT)
    fill(bufq, body, wq)
    fill(bufq.at[wcols // LANES :], body, nq)
    conv_all(bufq, (kwq, knq), qq)
    bufq[:, 0:EDGE, :] = bufq[:, BT:, :]
    outward = er[...]
    t = lax.broadcasted_iota(jnp.int32, (BT, BT), 0)
    s = lax.broadcasted_iota(jnp.int32, (BT, BT), 1)
    for g, (row, size, key) in enumerate(info):
        cols = slice(g * GW, (g + 1) * GW)
        q, k = qq[:, key : key + size], kk[:, key : key + size]
        weights = jnp.where(s <= t, dot_nt(q, k), 0.0).astype(BF16)
        y = dot(weights, up[:, cols]) + dot(q, hs[0, row : row + size, :])
        yl[:, cols] = y * dot(outward, table[:, cols])


def row_fades(groups, used, padded, place, sums, table):
    info, _ = group_rows(groups)
    factor = halves(jnp.exp(sums))
    heads = table.shape[0] // 2
    fades = [dot2(factor, table[:heads, g * GW : (g + 1) * GW]) for g in range(groups)]
    row = lax.broadcasted_iota(jnp.int32, (padded, GW), 0) + place * used
    masks = [row >= info[g][0] for g in range(1, groups)]

    def fade(k):
        out = jnp.broadcast_to(fades[0][k : k + 1], (padded, GW))
        for g in range(1, groups):
            out = jnp.where(masks[g - 1], fades[g][k : k + 1], out)
        return out

    return fade


def near_kernel(groups, chunk, where_ref, got, gather, unplace, place, table, prefix, sums, sent):
    used, padded = chunk
    count = got.shape[0] // padded
    lines = dot(gather[...], got[...]).astype(BF16)
    logs = dot(lines, unplace[...])
    sums[...] = logs
    fade = row_fades(groups, used, padded, where_ref[0], logs, table)
    held = jnp.zeros((padded, GW), F32)
    for k in range(count):
        part = slice(k * padded, (k + 1) * padded)
        prefix[part, :] = held
        held = fade(k) * held + got[part, :].astype(F32)
    total = halves(jnp.broadcast_to(jnp.sum(logs, axis=0, keepdims=True), (8, logs.shape[1])))
    line = (dot(total[0], place[:, 0:GW]) + dot(total[1], place[:, GW:]))[0:1]
    row = lax.broadcasted_iota(jnp.int32, held.shape, 0)
    sent[...] = jnp.where(row == used, line, held).astype(BF16)


def far_kernel(groups, chunk, where_ref, prefix, sums, unplace, table, *refs):
    used, padded = chunk
    others, out = refs[:-1], refs[-1]
    count = prefix.shape[0] // padded
    so_far = jnp.zeros((8, sums.shape[1]), F32)
    entering = jnp.zeros((padded, GW), F32)
    for n, other in enumerate(others):
        part = other[...].astype(F32)
        if n > 0:
            part = part * row_fades(groups, used, padded, where_ref[0], so_far, table)(0)
        entering += part
        so_far += dot(other[used : used + 8, :], unplace[...])[0:1]
    fade = row_fades(groups, used, padded, where_ref[0], sums[...], table)
    for k in range(count):
        part = slice(k * padded, (k + 1) * padded)
        out[part, :] = (prefix[part, :] + entering).astype(BF16)
        entering = fade(k) * entering


def project_kernel(groups, count, _, *refs):
    ins, (hin, gain, matrix, table, table_t) = refs[: 4 * count], refs[4 * count : 4 * count + 5]
    outs, (held, normed, near, arrived) = refs[4 * count + 5 : -4], refs[-4:]
    info, _ = group_rows(groups)
    share = ins[0].shape[0]

    tiles = arrived.shape[0]
    tile = matrix.shape[1] // tiles
    parts = [slice(t * tile, (t + 1) * tile) for t in range(tiles)]
    copies = [
        pltpu.make_async_copy(matrix.at[:, part], near.at[:, part], arrived.at[t])
        for t, part in enumerate(parts)
    ]
    for copy in copies:
        copy.start()
    for n in range(count):
        yl, qq, eR, gate = ins[4 * n : 4 * n + 4]
        reach = eR[...]
        squares = jnp.zeros((share, table.shape[0] // 2), F32)
        for g, (row, size, key) in enumerate(info):
            cols = slice(g * GW, (g + 1) * GW)
            outer = dot(qq[:, key : key + size], hin[row : row + size, :])
            y = yl[:, cols] + outer * dot(reach, table[:, cols])
            gated = y * silu(gate[:, cols].astype(F32))
            held[:, cols] = gated
            squares += dot2(halves(gated * gated), table_t[cols, :])
        scale = halves(lax.rsqrt(squares * (1.0 / CH) + EPS))
        for g in range(groups):
            cols = slice(g * GW, (g + 1) * GW)
            spread = dot2(scale, table[: table.shape[0] // 2, cols])
            unit = held[:, cols] * spread * gain[:, cols].astype(F32)
            normed[n * share : (n + 1) * share, cols] = unit.astype(BF16)

    half = outs[0].shape[0]
    for copy, part in zip(copies, parts):
        copy.wait()
        p = dot(normed[...], near[:, part]).astype(BF16)
        for n, out in enumerate(outs):
            out[:, part] = p[n * half : (n + 1) * half]


def place_kernel(unpick, back, out):
    out[...] = dot(unpick[...], back[...]).astype(BF16)


def norm_kernel(res, own, one, two, gain, after, x):
    total = own[...].astype(F32) + one[...].astype(F32) + two[...].astype(F32)
    mixed = (res[...].astype(F32) + total).astype(BF16)
    after[...] = mixed
    rows = mixed.astype(F32)
    scale = lax.rsqrt(jnp.mean(rows * rows, axis=1, keepdims=True) + EPS)
    x[...] = (rows * scale * gain[...].astype(F32)).astype(BF16)


def last_kernel(own_t, t1, t2, after_t, own_b, b1, b2, after_b, out):
    half = own_t.shape[0]
    for at, (own, one, two, after) in (
        (0, (own_t, t1, t2, after_t)),
        (half, (own_b, b1, b2, after_b)),
    ):
        total = own[...].astype(F32) + one[...].astype(F32) + two[...].astype(F32)
        out[at : at + half, :] = (after[...].astype(F32) + 0.5 * total).astype(BF16)


def pair_kernel(one, two, out):
    out[...] = (one[...].astype(F32) + two[...].astype(F32)).astype(BF16)


def feed_kernel(count, *refs):
    xs, (gate, up, down) = refs[:count], refs[count : count + 3]
    outs, total = refs[count + 3 : 2 * count + 3], refs[2 * count + 3]
    j = pl.program_id(0)
    x = jnp.concatenate([r[...] for r in xs], axis=0) if count > 1 else xs[0][...]
    hidden = (silu(dot(x, gate[...])) * dot(x, up[...])).astype(BF16)
    added = dot_nt(hidden, down[...])

    @pl.when(j == 0)
    def _():
        total[...] = added

    @pl.when(j > 0)
    def _():
        total[...] = total[...] + added

    @pl.when(j == pl.num_programs(0) - 1)
    def _():
        half = xs[0].shape[0]
        for n, out in enumerate(outs):
            out[...] = total[n * half : (n + 1) * half, :].astype(BF16)


def params(limit=VMEM_LIMIT):
    return pltpu.CompilerParams(dimension_semantics=("arbitrary",), vmem_limit_bytes=limit)


def cost(flops, moved):
    return pl.CostEstimate(flops=int(flops), bytes_accessed=int(moved), transcendentals=0)


def fixed(a):
    return pl.BlockSpec(a.shape, lambda *_: (0,) * a.ndim)


def whole(kernel, out_shapes, *args, flops=2e8):
    return pl.pallas_call(
        kernel,
        out_shape=out_shapes,
        compiler_params=pltpu.CompilerParams(vmem_limit_bytes=SMALL_LIMIT),
        cost_estimate=cost(flops, sum(a.size * 2 for a in args)),
    )(*args)


def ring(value, axis, step):
    count = lax.axis_size(axis)
    return lax.ppermute(value, axis, [(i, (i + step) % count) for i in range(count)])


def feed(xs, weights, tile=256):
    half, width = xs[0].shape
    inner = weights.shape[1] // 3
    tiles = inner // tile
    rows = half * len(xs)
    shape = jax.ShapeDtypeStruct((half, width), BF16)
    part = lambda n: pl.BlockSpec((width, tile), lambda j: (0, n * tiles + j))
    return pl.pallas_call(
        functools.partial(feed_kernel, len(xs)),
        grid=(tiles,),
        in_specs=[fixed(a) for a in xs] + [part(0), part(1), part(2)],
        out_specs=[pl.BlockSpec((half, width), lambda j: (0, 0))] * len(xs),
        out_shape=[shape] * len(xs),
        scratch_shapes=[pltpu.VMEM((rows, width), F32)],
        compiler_params=params(FEED_LIMIT),
        cost_estimate=cost(6 * rows * width * inner, weights.size * 2),
    )(*xs, weights, weights, weights)


def collect(own, left, right, opposite):
    send = lambda value, step: ring(value, "tp", step)
    from_left = send(opposite[0], 1)
    from_right = send(opposite[1], -1)
    bottom_left = send(right[1], 1)
    top_right = send(left[0], -1)
    shape = jax.ShapeDtypeStruct(own[0].shape, BF16)
    to_right = whole(pair_kernel, shape, right[0], from_left)
    to_left = whole(pair_kernel, shape, left[1], from_right)
    top_left = send(to_right, 1)
    bottom_right = send(to_left, -1)
    return (own[0], top_left, top_right), (own[1], bottom_left, bottom_right)


def on_device(
    residual, value_projected, gate_projected, wide_key_rows, wide_query_rows, narrow_key_rows,
    narrow_query_rows, step_before_softplus, extra_log_decay, log_decay_rate, value_kernel,
    wide_key_kernel, wide_query_kernel, narrow_key_kernel, narrow_query_kernel, head_norm_gain,
    output_matrix, feedforward_norm_gain, gate_matrix, up_matrix, down_matrix,
):
    sp, tp = lax.axis_size("sp"), lax.axis_size("tp")
    length, inner = value_projected.shape
    heads = inner // CH
    groups = heads // PER
    wcols, ncols = wide_key_rows.shape[1], narrow_key_rows.shape[1]
    keys = wcols + ncols
    width = output_matrix.shape[1]
    _, rows = group_rows(groups)
    near = 8 if sp % 8 == 0 else 2
    used = rows // near
    padded = -(-(used + 8) // 16) * 16
    chunk = (used, padded)
    blocks = length // BT
    me_sp, me_tp = lax.axis_index("sp"), lax.axis_index("tp")

    struct = jax.ShapeDtypeStruct
    table_np = (np.arange(heads)[:, None] == np.arange(inner)[None] // CH).astype(np.float32)
    table = jnp.asarray(np.concatenate([table_np, table_np]), BF16)
    table_t = jnp.asarray(table_np.T, BF16)
    place_np = np.zeros((heads, 2 * GW), np.float32)
    place_np[np.arange(heads), np.arange(heads)] = 1
    place_np[np.arange(heads), GW + heads + np.arange(heads)] = 1
    unplace_np = (place_np[:, :GW] + place_np[:, GW:]).T
    place, unplace = jnp.asarray(place_np, BF16), jnp.asarray(unplace_np, BF16)
    slot = np.arange(near * padded)
    pick_np = (
        (slot % padded < used)[:, None]
        & ((slot // padded * used + slot % padded)[:, None] == np.arange(rows)[None])
    ).astype(np.float32)
    pick, unpick = jnp.asarray(pick_np, BF16), jnp.asarray(pick_np.T, BF16)
    gather = jnp.asarray(
        (np.arange(near)[:, None] * padded + used == slot[None]).astype(np.float32), BF16
    )

    rowed = (
        value_projected, wide_key_rows, narrow_key_rows, wide_query_rows, narrow_query_rows
    )

    def joined(arrays, specs):
        shape = (specs[0].block_shape[0], sum(a.shape[1] for a in arrays))
        return pl.pallas_call(
            join_kernel,
            grid=(1,),
            in_specs=specs,
            out_specs=pl.BlockSpec(shape, lambda i: (0, 0)),
            out_shape=struct(shape, BF16),
            compiler_params=params(),
            cost_estimate=cost(1e6, 1e6),
        )(*arrays)

    ends = [pl.BlockSpec((EDGE, a.shape[1]), lambda i: (length // EDGE - 1, 0)) for a in rowed]
    edge = joined(rowed, ends)
    rim = lax.ppermute(edge, "sp", [(i, i + 1) for i in range(sp - 1)])

    mats = (gate_matrix, up_matrix, down_matrix)
    weights = joined(mats, [fixed(a) for a in mats])
    gain, ff_gain = head_norm_gain.reshape(1, inner), feedforward_norm_gain.reshape(1, width)
    rim, gain, ff_gain, weights = lax.optimization_barrier((rim, gain, ff_gain, weights))
    row_spec = lambda w: pl.BlockSpec((BT, w), lambda i: (i, 0))
    planes = lambda w: pltpu.VMEM((w // LANES, EDGE + BT, LANES), F32)
    time_spec = pl.BlockSpec((heads, BT), lambda i: (0, i))
    rate = log_decay_rate.reshape(1, heads)
    up, kk, er, eR, hs, st = pl.pallas_call(
        functools.partial(states_kernel, groups, chunk),
        grid=(blocks,),
        in_specs=[
            pl.BlockSpec(memory_space=pltpu.VMEM), row_spec(inner), row_spec(wcols), row_spec(ncols), time_spec,
            time_spec, fixed(rate), fixed(value_kernel), fixed(wide_key_kernel),
            fixed(narrow_key_kernel), fixed(table), fixed(place), fixed(pick),
        ],
        out_specs=[
            row_spec(inner), row_spec(keys), row_spec(2 * heads), row_spec(2 * heads),
            pl.BlockSpec((1, rows, GW), lambda i: (i, 0, 0)),
            pl.BlockSpec((near * padded, GW), lambda i: (0, 0)),
        ],
        out_shape=[
            struct((length, inner), BF16), struct((length, keys), BF16),
            struct((length, 2 * heads), BF16), struct((length, 2 * heads), BF16),
            struct((blocks, rows, GW), BF16), struct((near * padded, GW), BF16),
        ],
        scratch_shapes=[
            planes(inner), planes(keys),
            pltpu.VMEM((rows, GW), F32), pltpu.VMEM((heads, BT), F32),
        ],
        compiler_params=params(),
        cost_estimate=cost(8e9, 6e6),
    )(
        rim, value_projected, wide_key_rows, narrow_key_rows, step_before_softplus.T,
        extra_log_decay.T, rate, value_kernel, wide_key_kernel, narrow_key_kernel, table, place,
        pick,
    )

    seats = [[q + n for n in range(near)] for q in range(0, sp, near)]
    exchange = lambda a: lax.all_to_all(a, "sp", 0, 0, axis_index_groups=seats, tiled=True)
    got = exchange(st)
    inner_call = pl.pallas_call(
        functools.partial(inner_kernel, groups),
        grid=(blocks,),
        in_specs=[
            fixed(rim), row_spec(wcols), row_spec(ncols), fixed(wide_query_kernel),
            fixed(narrow_query_kernel), row_spec(keys), row_spec(inner), row_spec(2 * heads),
            pl.BlockSpec((1, rows, GW), lambda i: (i, 0, 0)), fixed(table),
        ],
        out_specs=[row_spec(inner), row_spec(keys)],
        out_shape=[struct((length, inner), F32), struct((length, keys), BF16)],
        scratch_shapes=[planes(keys)],
        compiler_params=params(),
        cost_estimate=cost(8e9, 6e6),
    )
    smem = pl.BlockSpec(memory_space=pltpu.SMEM)
    vmem = pl.BlockSpec(memory_space=pltpu.VMEM)
    seat = lax.rem(me_sp, near).reshape(1)
    prefix, sums, sent = pl.pallas_call(
        functools.partial(near_kernel, groups, chunk),
        in_specs=[smem] + [vmem] * 5,
        out_shape=[struct(st.shape, F32), struct((near, heads), F32), struct((padded, GW), BF16)],
        compiler_params=pltpu.CompilerParams(vmem_limit_bytes=SMALL_LIMIT),
        cost_estimate=cost(1e9, 1e6),
    )(seat, got, gather, unplace, place, table)
    weights, sent = lax.optimization_barrier((weights, sent))
    weights = lax.all_gather(weights, "sp", axis=0, tiled=True)
    weights = pltpu.with_memory_space_constraint(weights, pltpu.HBM)
    others = [
        lax.ppermute(sent, "sp", [(i, i + near * n) for i in range(sp - near * n)])
        for n in range(1, sp // near)
    ]
    entered = pl.pallas_call(
        functools.partial(far_kernel, groups, chunk),
        in_specs=[smem] + [vmem] * (4 + len(others)),
        out_shape=struct(st.shape, BF16),
        compiler_params=pltpu.CompilerParams(vmem_limit_bytes=SMALL_LIMIT),
        cost_estimate=cost(1e9, 1e6),
    )(seat, prefix, sums, unplace, table, *others)
    er, entered = lax.optimization_barrier((er, entered))
    back = exchange(entered)
    yl, qq = inner_call(
        rim, wide_query_rows, narrow_query_rows, wide_query_kernel, narrow_query_kernel, kk, up,
        er, hs, table,
    )
    far = [
        pltpu.with_memory_space_constraint(a, pltpu.HBM) for a in (yl, qq, eR, gate_projected, output_matrix)
    ]
    hin = whole(place_kernel, struct((rows, GW), BF16), unpick, back)

    share = length // tp
    half = share // 2
    tile = 512

    def project(*offsets):
        count = len(offsets)
        mine = lambda w, n: pl.BlockSpec(
            (share, w), lambda i, me: (lax.rem(me[0] + offsets[n], tp), 0)
        )
        return pl.pallas_call(
            functools.partial(project_kernel, groups, count),
            grid_spec=pltpu.PrefetchScalarGridSpec(
                num_scalar_prefetch=1,
                grid=(1,),
                in_specs=[mine(w, n) for n in range(count) for w in (inner, keys, 2 * heads, inner)]
                + [fixed(hin), fixed(gain), pl.BlockSpec(memory_space=pltpu.HBM)]
                + [fixed(table), fixed(table_t)],
                out_specs=[pl.BlockSpec((half, width), lambda i, o: (0, 0))] * (2 * count),
                scratch_shapes=[
                    pltpu.VMEM((share, inner), F32), pltpu.VMEM((count * share, inner), BF16),
                    pltpu.VMEM((inner, width), BF16), pltpu.SemaphoreType.DMA((width // tile,)),
                ],
            ),
            out_shape=[struct((half, width), BF16)] * (2 * count),
            compiler_params=params(FEED_LIMIT),
            cost_estimate=cost(2 * count * share * inner * width, 6e6),
        )(me_tp.reshape(1), *far[:4] * count, hin, gain, far[4], table, table_t)

    opposite, sides, own = project(2), project(1, 3), project(0)
    right, left = sides[:2], sides[2:]
    top, bottom = collect(own, left, right, opposite)
    pair = [struct((half, width), BF16)] * 2

    def norm(at, terms):
        same = pl.BlockSpec((half, width), lambda i: (0, 0))
        return pl.pallas_call(
            norm_kernel,
            grid=(1,),
            in_specs=[pl.BlockSpec((half, width), lambda i: (at, 0))]
            + [same] * 3
            + [fixed(ff_gain)],
            out_specs=[same] * 2,
            out_shape=pair,
            compiler_params=params(SMALL_LIMIT),
            cost_estimate=cost(1e9, 5 * half * width * 2),
        )(residual, *terms, ff_gain)

    (after_t, x_t), (after_b, x_b) = norm(0, top), norm(1, bottom)

    left_t, right_b = ring(x_t, "tp", 1), ring(x_b, "tp", -1)
    left_b, right_t = ring(x_b, "tp", 1), ring(x_t, "tp", -1)
    opp_t, opp_b = ring(left_t, "tp", 1), ring(right_b, "tp", -1)
    own = feed([x_t, x_b], weights)
    near = feed([left_t, left_b, right_t, right_b], weights)
    opposite = feed([opp_t, opp_b], weights)
    top, bottom = collect(own, near[:2], near[2:], opposite)
    return whole(
        last_kernel, struct((share, width), BF16), *top, after_t, *bottom, after_b
    )


def solution(mesh):
    rows = P(("grp", "sp"), "tp")
    in_specs = (P(("grp", "sp", "tp"), None),) + (rows,) * 8 + (P("tp"),) + (P(None, "tp"),) * 5
    in_specs += (P("tp"), P("tp", None), P()) + (P("sp", "tp"),) * 3
    return jax.shard_map(
        on_device,
        mesh=mesh,
        in_specs=in_specs,
        out_specs=P(("grp", "sp", "tp"), None),
        check_vma=False,
    )
```
